32 devices in a mesh: grp: 2 (over y), sp: 4 (over z), tp: 4 (over x, core).
Axes of the slice: x: 2, y: 2, z: 4, core: 2. Of those that a mesh axis runs over, the one named last changes fastest.
Arguments:
- tokens: bfloat16 [6144, 2048], P(('grp', 'sp'), 'tp'), parts along dimension 0, may hold values from -8 to 8
- norm_gain: float32 [2, 2048], replicated, may hold values from 0.1 to 1.9
- w_value: bfloat16 [2, 2048, 2048], P(None, 'sp', 'tp'), may hold values from -0.125 to 0.125
- w_gate: bfloat16 [2, 2048, 2048], P(None, 'sp', 'tp'), may hold values from -0.125 to 0.125
- taps: float32 [2, 31, 2048], P(None, None, 'tp'), may hold values from -2 to 2
- ln_gain: float32 [2, 2048], P(None, 'tp'), may hold values from 0.1 to 1.9
- ln_shift: float32 [2, 2048], P(None, 'tp'), may hold values from -3 to 3
- w_out: bfloat16 [2, 2048, 2048], P(None, 'sp', 'tp'), may hold values from -0.125 to 0.125
Outputs:
- stream_out: bfloat16 [6144, 2048], P(('grp', 'sp'), 'tp'), parts along dimension 0
The draws below stay inside these ranges and needn't reach their ends.
There are 2 independent parts, one for each index of `grp`. The reference program is written for one: setup_inputs(seed, part) draws one part's arguments, and reference() takes and returns one part's arrays. A program takes and returns all parts, laid end to end along the dimension named above; an argument that names none is the same for every part. Nothing has to cross between parts.
All inputs are finite; a program needn't handle non-finite values.
Results may differ from the reference program's by a relative error of at most 0.012.
Values may be sent and summed in bfloat16 or wider, within the bound.
A program may use at most 64 MiB of HBM per device.

```python
import jax
import jax.numpy as jnp
from jax import lax

D = 2048
C = 2048
KERNEL = 31
LAYERS = 2
TOKENS = 3072


def draw_tokens(key, part):
    first, second = jax.random.split(jax.random.fold_in(key, 11), 2)
    ramp = jnp.exp(jnp.linspace(-0.7, 0.7, D))
    rough = jnp.exp(jax.random.uniform(second, (D,), minval=-0.5, maxval=0.5))
    base = jnp.clip(jax.random.normal(first, (TOKENS, D)), -2.4, 2.4)
    return (base * ramp * rough).astype(jnp.bfloat16)


def draw_taps(key, part):
    first, second = jax.random.split(jax.random.fold_in(key, 23), 2)
    ramp = jnp.exp(jnp.linspace(-0.7, 0.7, C))
    rough = jnp.exp(jax.random.uniform(second, (C,), minval=-0.4, maxval=0.4))
    base = jnp.clip(jax.random.normal(first, (LAYERS, KERNEL, C)), -3.0, 3.0)
    return (base * KERNEL ** (-0.5) * ramp * rough).astype(jnp.float32)


def block_scale(stream_key, dims, cuts, smallest, top_value):
    def one(dim, blocks):
        draws = jax.random.uniform(jax.random.fold_in(jax.random.fold_in(stream_key, 6), dim), (blocks,), jnp.float32, smallest / len(cuts), top_value / len(cuts))
        return jnp.repeat(jnp.exp(draws), dims[dim] // blocks).reshape((-1,) + (1,) * (len(dims) - dim - 1))

    factor_of = one(*cuts[0])
    for cut in cuts[1:]:
        factor_of = factor_of * one(*cut)
    return factor_of


def normal_values(stream_key, shape, deviation, most, shards=(), dtype=jnp.bfloat16):
    array = deviation * jax.random.normal(stream_key, shape, jnp.float32)
    if shards:
        array = array * block_scale(stream_key, shape, shards, -0.22, 0.18)
    return jnp.clip(array, -most, most).astype(dtype)


def setup_inputs(seed: int = 0, part: int = 0) -> dict:
    keys = jax.random.split(jax.random.key(seed), 9)
    part_keys = jax.random.split(jax.random.fold_in(keys[8], part), 9)
    tokens = draw_tokens(jax.random.fold_in(jax.random.fold_in(keys[8], part), 71), part)
    norm_gain = jnp.clip(1.0 + 0.18 * jax.random.normal(keys[1], (LAYERS, D), jnp.float32), 0.1, 1.9)
    w_value = normal_values(keys[2], (LAYERS, D, C), D ** -0.5, 0.125, ((1, 4), (2, 4)))
    w_gate = normal_values(keys[3], (LAYERS, D, C), D ** -0.5, 0.125, ((1, 4), (2, 4)))
    taps = draw_taps(jax.random.fold_in(keys[8], 71), part)
    ln_gain = jnp.clip(1.0 + 0.18 * jax.random.normal(keys[5], (LAYERS, C), jnp.float32), 0.1, 1.9)
    ln_shift = normal_values(keys[6], (LAYERS, C), 0.5, 3.0, ((1, 4),), jnp.float32)
    w_out = normal_values(keys[7], (LAYERS, C, D), C ** -0.5, 0.125, ((1, 4), (2, 4)))
    return {"tokens": tokens, "norm_gain": norm_gain, "w_value": w_value, "w_gate": w_gate, "taps": taps, "ln_gain": ln_gain, "ln_shift": ln_shift, "w_out": w_out}


def reference(tokens, norm_gain, w_value, w_gate, taps, ln_gain, ln_shift, w_out):
    half = (KERNEL - 1) // 2
    stream = tokens
    for layer in range(LAYERS):
        wide = stream.astype(jnp.float32)
        meansq = lax.optimization_barrier(jnp.mean(wide * wide, axis=1, keepdims=True))
        normed = (wide * lax.rsqrt(meansq + 1e-06) * norm_gain[layer]).astype(jnp.bfloat16)
        value = jnp.dot(normed, w_value[layer], preferred_element_type=jnp.float32)
        gate = jnp.dot(normed, w_gate[layer], preferred_element_type=jnp.float32)
        glu = (value * jax.nn.sigmoid(gate)).astype(jnp.bfloat16)
        padded = jnp.pad(glu.astype(jnp.float32), ((half, half), (0, 0)))
        count = glu.shape[0]
        conv = jnp.zeros(glu.shape, jnp.float32)
        for step in range(KERNEL):
            conv = conv + taps[layer, step][None, :] * padded[step:step + count]
        mean_c = lax.optimization_barrier(jnp.mean(conv, axis=1, keepdims=True))
        var_c = lax.optimization_barrier(jnp.mean(conv * conv, axis=1, keepdims=True)) - mean_c * mean_c
        shaped = (conv - mean_c) * lax.rsqrt(var_c + 1e-05) * ln_gain[layer] + ln_shift[layer]
        act = jax.nn.silu(shaped).astype(jnp.bfloat16)
        update = jnp.dot(act, w_out[layer], preferred_element_type=jnp.float32)
        stream = (stream.astype(jnp.float32) + update).astype(jnp.bfloat16)
    return stream
```

```python
import functools

import jax
import jax.numpy as jnp
from jax import lax
from jax.experimental import pallas as pl
from jax.experimental.pallas import tpu as pltpu
from jax.sharding import PartitionSpec as P

MESH = pl.DeviceIdType.MESH
HALO = 16
LANES = 128
BLOCK = 64


def body(
    sizes,
    tokens,
    norm_gain,
    w_value,
    w_gate,
    taps_in,
    ln_gain,
    ln_shift,
    w_out,
    out,
    taps,
    weights,
    gathered,
    glu,
    conv,
    act,
    sums,
    stats,
    norms,
    load_sem,
    z_send,
    z_recv,
    y_send,
    y_recv,
    x_send,
    x_recv,
    s_send,
    s_recv,
    h_send,
    h_recv,
    n_send,
    n_recv,
):
    groups, n, tp, chunks, subs = sizes
    chips = tp // 2
    grp, sp, me = lax.axis_index("grp"), lax.axis_index("sp"), lax.axis_index("tp")
    chip, core = me // 2, me % 2
    partner = chip * 2 + 1 - core
    layers, depth, cols = w_value.shape
    kernel = taps_in.shape[0]
    half = (kernel - 1) // 2
    count = tokens.shape[0]
    rows = count // chunks
    width = cols * tp
    hops = n - 1
    f32, bf16 = jnp.float32, jnp.bfloat16

    def aligned(value, unit):
        return pl.multiple_of(value, unit)

    barrier = pltpu.get_barrier_semaphore()
    for off in range(1, tp):
        pl.semaphore_signal(
            barrier, inc=1, device_id={"tp": (me + off) % tp}, device_id_type=MESH
        )
    for off in range(1, groups):
        pl.semaphore_signal(
            barrier, inc=1, device_id={"grp": (grp + off) % groups}, device_id_type=MESH
        )

    @pl.when(sp > 0)
    def _():
        pl.semaphore_signal(barrier, inc=1, device_id={"sp": sp - 1}, device_id_type=MESH)

    @pl.when(sp < n - 1)
    def _():
        pl.semaphore_signal(barrier, inc=1, device_id={"sp": sp + 1}, device_id_type=MESH)

    qc = cols // subs
    total = layers * 3 * subs
    part = depth // groups
    span = 2 * hops

    def own_load(m):
        layer, j = m // (3 * subs), m % (3 * subs)
        if j < 2 * subs:
            source, q = (w_value, w_gate)[j % 2], j // 2
        else:
            source, q = w_out, j - 2 * subs
        return pltpu.make_async_copy(
            source.at[layer, :, pl.ds(q * qc, qc)],
            weights.at[m, pl.ds(aligned(sp * depth, 16), depth), :],
            load_sem.at[m],
        )

    taps_load = pltpu.make_async_copy(taps_in, taps, load_sem.at[total])
    for m in range(total):
        own_load(m).start()
    taps_load.start()

    def piece(block, m, quarter):
        return weights.at[m, pl.ds(aligned(block * depth + quarter * part, 16), part), :]

    def z_copy(way, m, hop, block):
        ref = piece(block, m, grp)
        return pltpu.make_async_remote_copy(
            src_ref=ref,
            dst_ref=ref,
            send_sem=z_send.at[way, m, hop],
            recv_sem=z_recv.at[way, m, hop],
            device_id={"sp": sp + 1 if way == 0 else sp - 1},
            device_id_type=MESH,
        )

    def y_copy(m, block, off, quarter):
        ref = piece(block, m, quarter)
        return pltpu.make_async_remote_copy(
            src_ref=ref,
            dst_ref=ref,
            send_sem=y_send.at[m, block, off - 1],
            recv_sem=y_recv.at[m, block, off - 1],
            device_id={"grp": (grp + off) % groups},
            device_id_type=MESH,
        )

    last_up = jnp.maximum(sp - 1, 0)
    last_down = jnp.maximum(n - 2 - sp, 0)

    def weight_step(k):
        m, r, p = 2 * (k // span) + k % 2, (k % span) // 2, k % 2

        @pl.when(sp - (r + 1) >= 0)
        def _():
            block = sp - (r + 1)
            z_copy(0, m, r, block).wait_recv()

            @pl.when(sp < n - 1)
            def _():
                z_copy(0, m, r + 1, block).start()

            for off in range(1, groups):
                y_copy(m, block, off, grp).start()

        @pl.when(sp + (r + 1) < n)
        def _():
            block = sp + (r + 1)
            z_copy(1, m, r, block).wait_recv()

            @pl.when(sp > 0)
            def _():
                z_copy(1, m, r + 1, block).start()

            for off in range(1, groups):
                y_copy(m, block, off, grp).start()

        more = jnp.logical_and(p == 1, m + 2 < total)

        @pl.when(jnp.logical_and(r == last_up, jnp.logical_and(more, sp < n - 1)))
        def _():
            z_copy(0, m + 1, 0, sp).start()
            z_copy(0, m + 2, 0, sp).start()

        @pl.when(jnp.logical_and(r == last_down, jnp.logical_and(more, sp > 0)))
        def _():
            z_copy(1, m + 1, 0, sp).start()
            z_copy(1, m + 2, 0, sp).start()


    def weight_steps(low, high):
        lax.fori_loop(low, high, lambda k, c: (weight_step(k), c)[1], 0)

    def weight_wait(m):
        def wait(block, c):
            @pl.when(block != sp)
            def _():
                for off in range(1, groups):
                    y_copy(m, block, off, (grp + groups - off) % groups).wait_recv()

            return c

        lax.fori_loop(0, n, wait, 0)

    def chunk_rows(c):
        return pl.ds(aligned(c * rows, rows), rows)

    def x_copy(phase, c, source, slot, target):
        layer, sub = phase // (1 + subs), phase % (1 + subs)
        if sub == 0:
            lanes = pl.ds(aligned(source * cols, LANES), cols)
        else:
            lanes = pl.ds(aligned(source * cols + (sub - 1) * qc, LANES), qc)
        ref = gathered.at[2 * layer + min(sub, 1), chunk_rows(c), lanes]
        return pltpu.make_async_remote_copy(
            src_ref=ref,
            dst_ref=ref,
            send_sem=x_send.at[phase, c, slot],
            recv_sem=x_recv.at[phase, c, source],
            device_id={"tp": target},
            device_id_type=MESH,
        )

    def x_own(phase, c):
        for off in range(1, chips):
            x_copy(phase, c, me, off - 1, ((chip + off) % chips) * 2 + core).start()
        x_copy(phase, c, me, chips - 1, partner).start()

    def x_forward(phase, c):
        for off in range(1, chips):
            source = ((chip + off) % chips) * 2 + core
            x_copy(phase, c, source, 0, partner).wait_recv()
            x_copy(phase, c, source, chips - 1 + off, partner).start()

    def x_wait(phase, c):
        for off in range(chips):
            source = ((chip + off) % chips) * 2 + 1 - core
            x_copy(phase, c, source, 0, partner).wait_recv()

    def s_copy(phase, c, source, slot, target):
        ref = stats.at[phase, c, source]
        return pltpu.make_async_remote_copy(
            src_ref=ref,
            dst_ref=ref,
            send_sem=s_send.at[phase, c, slot],
            recv_sem=s_recv.at[phase, c, source],
            device_id={"tp": target},
            device_id_type=MESH,
        )

    def s_share(phase, c, values):
        stats[phase, c, me] = values.T[:8]
        for off in range(1, tp):
            s_copy(phase, c, me, off - 1, (me + off) % tp).start()

    def s_wait(phase, c):
        for off in range(1, tp):
            s_copy(phase, c, (me + off) % tp, 0, me).wait_recv()

    def s_total(phase, c):
        total = stats[phase, c, 0]
        for source in range(1, tp):
            total = total + stats[phase, c, source]
        return total

    def columns(rows_of_8):
        block = jnp.concatenate(rows_of_8, axis=0)
        return jnp.concatenate([block] * (LANES // block.shape[0]), axis=0).T

    def n_copy(which, source, slot, target):
        return pltpu.make_async_remote_copy(
            src_ref=(ln_gain, ln_shift)[which],
            dst_ref=norms.at[which, source],
            send_sem=n_send.at[which, slot],
            recv_sem=n_recv.at[which, source],
            device_id={"tp": target},
            device_id_type=MESH,
        )

    def h_copy(layer, q, way):
        if way == 0:
            source, target, device = count, 0, sp + 1
        else:
            source, target, device = HALO, HALO + count, sp - 1
        lanes = pl.ds(q * qc, qc)
        return pltpu.make_async_remote_copy(
            src_ref=glu.at[layer, pl.ds(source, HALO), lanes],
            dst_ref=glu.at[layer, pl.ds(target, HALO), lanes],
            send_sem=h_send.at[layer, q, way],
            recv_sem=h_recv.at[layer, q, way],
            device_id={"sp": device},
            device_id_type=MESH,
        )

    mine = pl.ds(aligned(me * cols, LANES), cols)
    lane = lax.broadcasted_iota(jnp.int32, (rows, LANES), 1)

    def share_stream(layer, c, wide):
        gain = norm_gain[pl.ds(layer, 1), mine]
        gathered[2 * layer, chunk_rows(c), mine] = (wide * gain).astype(bf16)
        x_own(layer * (1 + subs), c)
        square = jnp.sum(wide * wide, axis=1, keepdims=True)
        s_share(2 * layer, c, jnp.where(lane == 0, square, 0.0))

    def loop(function):
        lax.fori_loop(0, chunks, lambda i, c: (function(i), c)[1], 0)

    def inner_first(i):
        return (1 + 2 * i) % chunks

    def ends_first(i):
        return (2 * i) % chunks

    for layer in range(layers):

        @pl.when(sp == 0)
        def _():
            glu[layer, pl.ds(0, HALO), :] = jnp.zeros((HALO, cols), bf16)

        @pl.when(sp == n - 1)
        def _():
            glu[layer, pl.ds(HALO + count, HALO), :] = jnp.zeros((HALO, cols), bf16)

    for m in range(2):
        own_load(m).wait()
    pl.semaphore_wait(
        barrier,
        tp - 1 + groups - 1 + (sp > 0).astype(jnp.int32) + (sp < n - 1).astype(jnp.int32),
    )
    for m in range(2):

        @pl.when(sp < n - 1)
        def _():
            z_copy(0, m, 0, sp).start()

        @pl.when(sp > 0)
        def _():
            z_copy(1, m, 0, sp).start()

    loop(lambda c: share_stream(0, c, tokens[chunk_rows(c), :].astype(f32)))
    for which in range(2):
        for off in range(1, tp):
            n_copy(which, me, off - 1, (me + off) % tp).start()
    norms[0, me] = ln_gain[...]
    norms[1, me] = ln_shift[...]
    for m in range(2, total):
        own_load(m).wait()
    taps_load.wait()

    done = [0]

    def share(goal):
        low = done[0]
        high = max(low, min(goal, total * hops))
        done[0] = high
        return lambda i: weight_steps(
            low + (high - low) * i // chunks, low + (high - low) * (i + 1) // chunks
        )

    def advance(goal):
        low = done[0]
        high = max(low, min(goal, total * hops))
        done[0] = high
        weight_steps(low, high)

    def gated(layer, q, steps, i):
        c = ends_first(i)
        if q == 0:
            s_wait(2 * layer, c)
        scale = lax.rsqrt(columns([s_total(2 * layer, c)])[:, :1] / width + 1e-06)
        block = gathered[2 * layer, chunk_rows(c), :]
        first = layer * 3 * subs + 2 * q
        value = jnp.dot(block, weights[first], preferred_element_type=f32) * scale
        gate = jnp.dot(block, weights[first + 1], preferred_element_type=f32) * (0.5 * scale)
        glu[layer, pl.ds(aligned(HALO + c * rows, HALO), rows), pl.ds(q * qc, qc)] = (
            value * (0.5 + 0.5 * jnp.tanh(gate))
        ).astype(bf16)

        @pl.when(jnp.logical_and(c == 0, sp > 0))
        def _():
            h_copy(layer, q, 1).start()

        @pl.when(jnp.logical_and(c == chunks - 1, sp < n - 1))
        def _():
            h_copy(layer, q, 0).start()

        steps(i)

    shift = HALO - half
    groups_of_8 = (kernel + shift + 7) // 8
    window = BLOCK + 8 * groups_of_8

    def convolve(layer, q, c):
        lane_blocks = qc // LANES

        def block(i, carry):
            base = aligned(c * rows + (i // lane_blocks) * BLOCK, BLOCK)
            inside = aligned((i % lane_blocks) * LANES, LANES)
            lanes = pl.ds(aligned(q * qc + inside, LANES), LANES)
            values = glu[layer, pl.ds(base, window), lanes].astype(f32)
            total = None
            for j in range(8):
                partial = None
                for g in range(groups_of_8):
                    tap = 8 * g + j - shift
                    if tap < 0 or tap >= kernel:
                        continue
                    term = taps[tap, pl.ds(layer, 1), lanes] * values[8 * g : 8 * g + BLOCK + 8]
                    partial = term if partial is None else partial + term
                piece_j = partial[j : j + BLOCK]
                total = piece_j if total is None else total + piece_j
            conv[pl.ds(base, BLOCK), pl.ds(inside, LANES)] = total
            return carry

        lax.fori_loop(0, rows // BLOCK * lane_blocks, block, 0)

    def mixed(layer, q, steps, i):
        c = inner_first(i)

        @pl.when(jnp.logical_and(c == 0, sp > 0))
        def _():
            h_copy(layer, q, 0).wait_recv()

        @pl.when(jnp.logical_and(c == chunks - 1, sp < n - 1))
        def _():
            h_copy(layer, q, 1).wait_recv()

        convolve(layer, q, c)
        whole = conv[chunk_rows(c), :]
        row_sum = jnp.sum(whole, axis=1, keepdims=True)
        lanes = pl.ds(aligned(me * cols + q * qc, LANES), qc)
        gathered[2 * layer + 1, chunk_rows(c), lanes] = (whole - row_sum / qc).astype(bf16)
        x_own(layer * (1 + subs) + 1 + q, c)
        square = jnp.sum(whole * whole, axis=1, keepdims=True)
        both = jnp.where(lane == q, row_sum, jnp.where(lane == 4, square, 0.0))
        if q > 0:
            both = both + sums[chunk_rows(c), :]
        if q < subs - 1:
            sums[chunk_rows(c), :] = both
        else:
            s_share(2 * layer + 1, c, both)
        steps(i)

    def arrive(phase, steps, i):
        c = i if phase == 0 else inner_first(i)
        steps(i)
        x_forward(phase, c)
        x_wait(phase, c)

    sublane = lax.broadcasted_iota(jnp.int32, (8, rows), 0)

    def activate(layer, steps, i):
        c = inner_first(i)
        phase = 2 * layer + 1
        x_forward(layer * (1 + subs) + subs, c)
        x_wait(layer * (1 + subs) + subs, c)
        s_wait(phase, c)
        total = s_total(phase, c)
        mean = total[0:1]
        for q in range(1, subs):
            mean = mean + total[q : q + 1]
        mean = mean / width
        inverse = lax.rsqrt(total[4:5] / width - mean * mean + 1e-05)
        offsets = [
            jnp.where(sublane == 4, inverse, (stats[phase, c, source] / qc - mean) * inverse)
            for source in range(tp)
        ]
        table = columns(offsets)
        for source in range(tp):
            for q in range(subs):
                lanes = pl.ds(source * cols + q * qc, qc)
                inside = pl.ds(q * qc, qc)
                gain = 0.5 * norms[0, source, pl.ds(layer, 1), inside]
                moved = 0.5 * norms[1, source, pl.ds(layer, 1), inside]
                offset = table[:, 8 * source + q : 8 * source + q + 1]
                block = gathered[phase, chunk_rows(c), lanes].astype(f32)
                shaped = (block * table[:, 4:5] + offset) * gain + moved
                act[chunk_rows(c), lanes] = (shaped + shaped * jnp.tanh(shaped)).astype(bf16)
        steps(i)

    def close(layer, q, steps, i):
        c = inner_first(i)
        update = jnp.dot(
            act[chunk_rows(c), :],
            weights[layer * 3 * subs + 2 * subs + q],
            preferred_element_type=f32,
        )
        source = tokens if layer == 0 else out
        lanes = pl.ds(q * qc, qc)
        out[chunk_rows(c), lanes] = (source[chunk_rows(c), lanes].astype(f32) + update).astype(bf16)
        if q == subs - 1 and layer + 1 < layers:
            share_stream(layer + 1, c, out[chunk_rows(c), :].astype(f32))
        steps(i)

    def need(m):
        return (m // 2 + 1) * span

    def part_of(steps):
        return steps * span // 6

    for layer in range(layers):
        first = layer * 3 * subs
        loop(functools.partial(arrive, layer * (1 + subs), share(done[0] + part_of(6))))
        if layer == 0:
            for which in range(2):
                for off in range(1, tp):
                    n_copy(which, (me + off) % tp, 0, me).wait_recv()
        for q in range(subs):
            advance(need(first + 2 * q + 1) + part_of(2))
            weight_wait(first + 2 * q)
            weight_wait(first + 2 * q + 1)
            loop(functools.partial(gated, layer, q, share(done[0] + part_of(1))))
            loop(functools.partial(mixed, layer, q, share(done[0] + part_of(1))))
            if q < subs - 1:
                loop(functools.partial(arrive, layer * (1 + subs) + 1 + q, share(done[0] + part_of(3))))
        last = first + 2 * subs
        advance(need(last + subs - 1) + 0)
        loop(functools.partial(activate, layer, share(done[0] + 0)))
        advance(need(last + subs - 1) + part_of(2))
        for q in range(subs):
            weight_wait(last + q)
            loop(functools.partial(close, layer, q, share(done[0])))
    advance(total * hops)

    def drain_weights(i, carry):
        m, block = i // n, i % n

        @pl.when(block <= sp)
        def _():
            @pl.when(sp < n - 1)
            def _():
                z_copy(0, m, sp - block, block).wait_send()

        @pl.when(block >= sp)
        def _():
            @pl.when(sp > 0)
            def _():
                z_copy(1, m, block - sp, block).wait_send()

        @pl.when(block != sp)
        def _():
            for off in range(1, groups):
                y_copy(m, block, off, grp).wait_send()

        return carry

    lax.fori_loop(0, total * n, drain_weights, 0)

    def drain_chunks(c, carry):
        for slot in range(tp - 1):
            for phase in range(layers * (1 + subs)):
                x_copy(phase, c, me, slot, partner).wait_send()
            for phase in range(2 * layers):
                s_copy(phase, c, me, slot, partner).wait_send()
        return carry

    lax.fori_loop(0, chunks, drain_chunks, 0)
    for which in range(2):
        for slot in range(tp - 1):
            n_copy(which, me, slot, partner).wait_send()
    for layer in range(layers):
        for q in range(subs):

            @pl.when(sp < n - 1)
            def _():
                h_copy(layer, q, 0).wait_send()

            @pl.when(sp > 0)
            def _():
                h_copy(layer, q, 1).wait_send()


def solution(mesh):
    groups, n, tp = mesh.shape["grp"], mesh.shape["sp"], mesh.shape["tp"]

    def shards(tokens, norm_gain, w_value, w_gate, taps, ln_gain, ln_shift, w_out):
        layers, depth, cols = w_value.shape
        count = tokens.shape[0]
        chunks = 3
        subs = 2 if cols % (2 * LANES) == 0 else 1
        pieces = layers * 3 * subs
        taps = jnp.transpose(taps, (1, 0, 2))
        rows = count // chunks
        vmem = pl.BlockSpec(memory_space=pltpu.VMEM)
        hbm = pl.BlockSpec(memory_space=pl.ANY)
        dma = pltpu.SemaphoreType.DMA
        return pl.pallas_call(
            functools.partial(body, (groups, n, tp, chunks, subs)),
            out_shape=jax.ShapeDtypeStruct((count, cols), jnp.bfloat16),
            in_specs=[vmem, vmem, hbm, hbm, hbm, vmem, vmem, hbm],
            out_specs=vmem,
            scratch_shapes=[
                pltpu.VMEM(taps.shape, jnp.float32),
                pltpu.VMEM((pieces, depth * n, cols // subs), jnp.bfloat16),
                pltpu.VMEM((2 * layers, count, cols * tp), jnp.bfloat16),
                pltpu.VMEM((layers, count + 2 * HALO, cols), jnp.bfloat16),
                pltpu.VMEM((count, cols // subs), jnp.float32),
                pltpu.VMEM((count, cols * tp), jnp.bfloat16),
                pltpu.VMEM((count, LANES), jnp.float32),
                pltpu.VMEM((2 * layers, chunks, tp, 8, rows), jnp.float32),
                pltpu.VMEM((2, tp, layers, cols), jnp.float32),
                dma((pieces + 1,)),
                dma((2, pieces, n - 1)),
                dma((2, pieces, n - 1)),
                dma((pieces, n, groups - 1)),
                dma((pieces, n, groups - 1)),
                dma((layers * (1 + subs), chunks, tp - 1)),
                dma((layers * (1 + subs), chunks, tp)),
                dma((2 * layers, chunks, tp - 1)),
                dma((2 * layers, chunks, tp)),
                dma((layers, subs, 2)),
                dma((layers, subs, 2)),
                dma((2, tp - 1)),
                dma((2, tp)),
            ],
            compiler_params=pltpu.CompilerParams(
                collective_id=0, has_side_effects=True, vmem_limit_bytes=60 * 1024 * 1024
            ),
        )(tokens, norm_gain, w_value, w_gate, taps, ln_gain, ln_shift, w_out)

    return jax.shard_map(
        shards,
        mesh=mesh,
        in_specs=(
            P(("grp", "sp"), "tp"),
            P(),
            P(None, "sp", "tp"),
            P(None, "sp", "tp"),
            P(None, None, "tp"),
            P(None, "tp"),
            P(None, "tp"),
            P(None, "sp", "tp"),
        ),
        out_specs=P(("grp", "sp"), "tp"),
        check_vma=False,
    )
```

```python
import functools

import jax
import jax.numpy as jnp
from jax import lax
from jax.experimental import pallas as pl
from jax.experimental.pallas import tpu as pltpu
from jax.sharding import PartitionSpec as P

MESH = pl.DeviceIdType.MESH
HALO = 16
LANES = 128
BLOCK = 64


def body(
    sizes,
    tokens_in,
    gain_in,
    w_value,
    w_gate,
    taps_in,
    ln_gain,
    ln_shift,
    w_out,
    out,
    tokens,
    norm_gain,
    taps,
    weights,
    gathered,
    glu,
    conv,
    act,
    sums,
    stats,
    norms,
    load_sem,
    z_send,
    z_recv,
    y_send,
    y_recv,
    x_send,
    x_recv,
    s_send,
    s_recv,
    h_send,
    h_recv,
    n_send,
    n_recv,
):
    groups, n, tp, chunks, subs = sizes
    chips = tp // 2
    grp, sp, me = lax.axis_index("grp"), lax.axis_index("sp"), lax.axis_index("tp")
    chip, core = me // 2, me % 2
    partner = chip * 2 + 1 - core
    layers, depth, cols = w_value.shape
    kernel = taps_in.shape[0]
    half = (kernel - 1) // 2
    count = tokens_in.shape[0]
    rows = count // chunks
    width = cols * tp
    hops = n - 1
    f32, bf16 = jnp.float32, jnp.bfloat16

    def aligned(value, unit):
        return pl.multiple_of(value, unit)

    barrier = pltpu.get_barrier_semaphore()
    for off in range(1, tp):
        pl.semaphore_signal(
            barrier, inc=1, device_id={"tp": (me + off) % tp}, device_id_type=MESH
        )
    for off in range(1, groups):
        pl.semaphore_signal(
            barrier, inc=1, device_id={"grp": (grp + off) % groups}, device_id_type=MESH
        )

    @pl.when(sp > 0)
    def _():
        pl.semaphore_signal(barrier, inc=1, device_id={"sp": sp - 1}, device_id_type=MESH)

    @pl.when(sp < n - 1)
    def _():
        pl.semaphore_signal(barrier, inc=1, device_id={"sp": sp + 1}, device_id_type=MESH)

    qc = cols // subs
    total = layers * 3 * subs
    part = depth // groups
    span = 2 * hops

    def own_load(m):
        layer, j = m // (3 * subs), m % (3 * subs)
        if j < 2 * subs:
            source, q = (w_value, w_gate)[j % 2], j // 2
        else:
            source, q = w_out, j - 2 * subs
        return pltpu.make_async_copy(
            source.at[layer, :, pl.ds(q * qc, qc)],
            weights.at[m, pl.ds(aligned(sp * depth, 16), depth), :],
            load_sem.at[0 if m < 2 else 1],
        )

    tokens_load = pltpu.make_async_copy(tokens_in, tokens, load_sem.at[2])
    gain_load = pltpu.make_async_copy(gain_in, norm_gain, load_sem.at[3])
    taps_load = pltpu.make_async_copy(taps_in, taps, load_sem.at[4])
    own_load(0).start()
    own_load(1).start()
    tokens_load.start()
    gain_load.start()

    def piece(block, m, quarter):
        return weights.at[m, pl.ds(aligned(block * depth + quarter * part, 16), part), :]

    def z_copy(way, m, block):
        ref = piece(block, m, grp)
        return pltpu.make_async_remote_copy(
            src_ref=ref,
            dst_ref=ref,
            send_sem=z_send.at[way],
            recv_sem=z_recv.at[m, block - way],
            device_id={"sp": sp + 1 if way == 0 else sp - 1},
            device_id_type=MESH,
        )

    def y_copy(m, block, off, quarter):
        ref = piece(block, m, quarter)
        return pltpu.make_async_remote_copy(
            src_ref=ref,
            dst_ref=ref,
            send_sem=y_send.at[off - 1],
            recv_sem=y_recv.at[m, off - 1],
            device_id={"grp": (grp + off) % groups},
            device_id_type=MESH,
        )

    last_up = jnp.maximum(sp - 1, 0)
    last_down = jnp.maximum(n - 2 - sp, 0)

    def weight_step(k):
        m, r, p = 2 * (k // span) + k % 2, (k % span) // 2, k % 2

        @pl.when(sp - (r + 1) >= 0)
        def _():
            block = sp - (r + 1)
            z_copy(0, m, block).wait_recv()

            @pl.when(sp < n - 1)
            def _():
                z_copy(0, m, block).start()

            for off in range(1, groups):
                y_copy(m, block, off, grp).start()

        @pl.when(sp + (r + 1) < n)
        def _():
            block = sp + (r + 1)
            z_copy(1, m, block).wait_recv()

            @pl.when(sp > 0)
            def _():
                z_copy(1, m, block).start()

            for off in range(1, groups):
                y_copy(m, block, off, grp).start()

        more = jnp.logical_and(p == 1, m + 2 < total)

        @pl.when(jnp.logical_and(r == last_up, jnp.logical_and(more, sp < n - 1)))
        def _():
            z_copy(0, m + 1, sp).start()
            z_copy(0, m + 2, sp).start()

        @pl.when(jnp.logical_and(r == last_down, jnp.logical_and(more, sp > 0)))
        def _():
            z_copy(1, m + 1, sp).start()
            z_copy(1, m + 2, sp).start()


    def weight_steps(low, high):
        lax.fori_loop(low, high, lambda k, c: (weight_step(k), c)[1], 0)

    def landed(ref, sem):
        pltpu.make_async_copy(ref, ref, sem).wait()

    def weight_wait(m):
        for off in range(1, groups):
            landed(weights.at[m, pl.ds(0, hops * part), :], y_recv.at[m, off - 1])

    def chunk_rows(c):
        return pl.ds(aligned(c * rows, rows), rows)

    def x_lanes(phase, source):
        sub = phase % (1 + subs)
        if sub == 0:
            return pl.ds(aligned(source * cols, LANES), cols)
        return pl.ds(aligned(source * cols + (sub - 1) * qc, LANES), qc)

    def x_copy(phase, c, source, slot, target):
        layer, sub = phase // (1 + subs), phase % (1 + subs)
        ref = gathered.at[2 * layer + min(sub, 1), chunk_rows(c), x_lanes(phase, source)]
        return pltpu.make_async_remote_copy(
            src_ref=ref,
            dst_ref=ref,
            send_sem=x_send,
            recv_sem=x_recv.at[phase, c, slot],
            device_id={"tp": target},
            device_id_type=MESH,
        )

    def x_own(phase, c):
        for off in range(1, chips):
            x_copy(phase, c, me, off, ((chip + off) % chips) * 2 + core).start()
        x_copy(phase, c, me, 0, partner).start()

    def x_forward(phase, c):
        for off in range(1, chips):
            source = ((chip + chips - off) % chips) * 2 + core
            x_copy(phase, c, source, off, partner).wait_recv()
            x_copy(phase, c, source, 0, partner).start()

    def x_wait(phase, c):
        ref = gathered.at[0, pl.ds(0, rows), pl.ds(0, chips * (cols if phase % (1 + subs) == 0 else qc))]
        landed(ref, x_recv.at[phase, c, 0])

    def s_copy(phase, c, source, target):
        ref = stats.at[phase, c, source]
        return pltpu.make_async_remote_copy(
            src_ref=ref,
            dst_ref=ref,
            send_sem=s_send,
            recv_sem=s_recv.at[phase, c],
            device_id={"tp": target},
            device_id_type=MESH,
        )

    def s_share(phase, c, values):
        stats[phase, c, me] = values.T[:8]
        for off in range(1, tp):
            s_copy(phase, c, me, (me + off) % tp).start()

    def s_wait(phase, c):
        landed(stats.at[phase, c, pl.ds(0, tp - 1)], s_recv.at[phase, c])

    def s_total(phase, c):
        total = stats[phase, c, 0]
        for source in range(1, tp):
            total = total + stats[phase, c, source]
        return total

    def columns(rows_of_8):
        block = jnp.concatenate(rows_of_8, axis=0)
        return jnp.concatenate([block] * (LANES // block.shape[0]), axis=0).T

    def n_load(which):
        source = (ln_gain, ln_shift)[which]
        return pltpu.make_async_copy(source, norms.at[which, me], load_sem.at[5])

    def n_copy(which, target):
        return pltpu.make_async_remote_copy(
            src_ref=(ln_gain, ln_shift)[which],
            dst_ref=norms.at[which, me],
            send_sem=n_send,
            recv_sem=n_recv,
            device_id={"tp": target},
            device_id_type=MESH,
        )

    def h_copy(layer, q, way):
        if way == 0:
            source, target, device = count, 0, sp + 1
        else:
            source, target, device = HALO, HALO + count, sp - 1
        lanes = pl.ds(q * qc, qc)
        return pltpu.make_async_remote_copy(
            src_ref=glu.at[layer, pl.ds(source, HALO), lanes],
            dst_ref=glu.at[layer, pl.ds(target, HALO), lanes],
            send_sem=h_send.at[way],
            recv_sem=h_recv.at[layer, q, way],
            device_id={"sp": device},
            device_id_type=MESH,
        )

    mine = pl.ds(aligned(me * cols, LANES), cols)
    lane = lax.broadcasted_iota(jnp.int32, (rows, LANES), 1)

    def share_stream(layer, c, wide):
        gain = norm_gain[pl.ds(layer, 1), mine]
        gathered[2 * layer, chunk_rows(c), mine] = (wide * gain).astype(bf16)
        x_own(layer * (1 + subs), c)
        square = jnp.sum(wide * wide, axis=1, keepdims=True)
        s_share(2 * layer, c, jnp.where(lane == 0, square, 0.0))

    def loop(function):
        lax.fori_loop(0, chunks, lambda i, c: (function(i), c)[1], 0)

    def inner_first(i):
        return (1 + 2 * i) % chunks

    def ends_first(i):
        return (2 * i) % chunks

    for layer in range(layers):

        @pl.when(sp == 0)
        def _():
            glu[layer, pl.ds(0, HALO), :] = jnp.zeros((HALO, cols), bf16)

        @pl.when(sp == n - 1)
        def _():
            glu[layer, pl.ds(HALO + count, HALO), :] = jnp.zeros((HALO, cols), bf16)

    landed(weights.at[pl.ds(0, 2), pl.ds(0, depth), :], load_sem.at[0])
    pl.semaphore_wait(
        barrier,
        tp - 1 + groups - 1 + (sp > 0).astype(jnp.int32) + (sp < n - 1).astype(jnp.int32),
    )
    for m in range(2):

        @pl.when(sp < n - 1)
        def _():
            z_copy(0, m, sp).start()

        @pl.when(sp > 0)
        def _():
            z_copy(1, m, sp).start()

    for m in range(2, total):
        own_load(m).start()
    taps_load.start()
    for which in range(2):
        n_load(which).start()
    tokens_load.wait()
    gain_load.wait()
    loop(lambda c: share_stream(0, c, tokens[chunk_rows(c), :].astype(f32)))
    for which in range(2):
        for off in range(1, tp):
            n_copy(which, (me + off) % tp).start()
    landed(weights.at[pl.ds(2, total - 2), pl.ds(0, depth), :], load_sem.at[1])
    taps_load.wait()
    landed(norms.at[:, 0], load_sem.at[5])

    done = [0]

    def share(goal):
        low = done[0]
        high = max(low, min(goal, total * hops))
        done[0] = high
        return lambda i: weight_steps(
            low + (high - low) * i // chunks, low + (high - low) * (i + 1) // chunks
        )

    def advance(goal):
        low = done[0]
        high = max(low, min(goal, total * hops))
        done[0] = high
        weight_steps(low, high)

    def gated(layer, q, steps, i):
        c = ends_first(i)
        if q == 0:
            s_wait(2 * layer, c)
        scale = lax.rsqrt(columns([s_total(2 * layer, c)])[:, :1] / width + 1e-06)
        block = gathered[2 * layer, chunk_rows(c), :]
        first = layer * 3 * subs + 2 * q
        value = jnp.dot(block, weights[first], preferred_element_type=f32) * scale
        gate = jnp.dot(block, weights[first + 1], preferred_element_type=f32) * (0.5 * scale)
        glu[layer, pl.ds(aligned(HALO + c * rows, HALO), rows), pl.ds(q * qc, qc)] = (
            value * (0.5 + 0.5 * jnp.tanh(gate))
        ).astype(bf16)

        @pl.when(jnp.logical_and(c == 0, sp > 0))
        def _():
            h_copy(layer, q, 1).start()

        @pl.when(jnp.logical_and(c == chunks - 1, sp < n - 1))
        def _():
            h_copy(layer, q, 0).start()

        steps(i)

    shift = HALO - half
    groups_of_8 = (kernel + shift + 7) // 8
    window = BLOCK + 8 * groups_of_8

    def convolve(layer, q, c):
        lane_blocks = qc // LANES

        def block(i, carry):
            base = aligned(c * rows + (i // lane_blocks) * BLOCK, BLOCK)
            inside = aligned((i % lane_blocks) * LANES, LANES)
            lanes = pl.ds(aligned(q * qc + inside, LANES), LANES)
            values = glu[layer, pl.ds(base, window), lanes].astype(f32)
            total = None
            for j in range(8):
                partial = None
                for g in range(groups_of_8):
                    tap = 8 * g + j - shift
                    if tap < 0 or tap >= kernel:
                        continue
                    term = taps[tap, pl.ds(layer, 1), lanes] * values[8 * g : 8 * g + BLOCK + 8]
                    partial = term if partial is None else partial + term
                piece_j = partial[j : j + BLOCK]
                total = piece_j if total is None else total + piece_j
            conv[pl.ds(base, BLOCK), pl.ds(inside, LANES)] = total
            return carry

        lax.fori_loop(0, rows // BLOCK * lane_blocks, block, 0)

    def mixed(layer, q, forward, steps, i):
        c = inner_first(i)

        @pl.when(jnp.logical_and(c == 0, sp > 0))
        def _():
            h_copy(layer, q, 0).wait_recv()

        @pl.when(jnp.logical_and(c == chunks - 1, sp < n - 1))
        def _():
            h_copy(layer, q, 1).wait_recv()

        convolve(layer, q, c)
        whole = conv[chunk_rows(c), :]
        row_sum = jnp.sum(whole, axis=1, keepdims=True)
        lanes = pl.ds(aligned(me * cols + q * qc, LANES), qc)
        gathered[2 * layer + 1, chunk_rows(c), lanes] = (whole - row_sum / qc).astype(bf16)
        x_own(layer * (1 + subs) + 1 + q, c)
        square = jnp.sum(whole * whole, axis=1, keepdims=True)
        both = jnp.where(lane == q, row_sum, jnp.where(lane == 4, square, 0.0))
        if q > 0:
            both = both + sums[chunk_rows(c), :]
        if q < subs - 1:
            sums[chunk_rows(c), :] = both
        else:
            s_share(2 * layer + 1, c, both)
        if forward is not None:
            x_forward(forward, c)
        steps(i)

    def arrive(phase, steps, i):
        c = i if phase == 0 else inner_first(i)
        steps(i)
        x_forward(phase, c)
        x_wait(phase, c)

    sublane = lax.broadcasted_iota(jnp.int32, (8, rows), 0)

    def activate(layer, steps, i):
        c = inner_first(i)
        phase = 2 * layer + 1
        x_forward(layer * (1 + subs) + subs, c)
        s_wait(phase, c)
        for q in range(0 if layer else subs - 1, subs):
            x_wait(layer * (1 + subs) + 1 + q, c)
        total = s_total(phase, c)
        mean = total[0:1]
        for q in range(1, subs):
            mean = mean + total[q : q + 1]
        mean = mean / width
        inverse = lax.rsqrt(total[4:5] / width - mean * mean + 1e-05)
        offsets = [
            jnp.where(sublane == 4, inverse, (stats[phase, c, source] / qc - mean) * inverse)
            for source in range(tp)
        ]
        table = columns(offsets)
        for source in range(tp):
            for q in range(subs):
                lanes = pl.ds(source * cols + q * qc, qc)
                inside = pl.ds(q * qc, qc)
                gain = 0.5 * norms[0, source, pl.ds(layer, 1), inside]
                moved = 0.5 * norms[1, source, pl.ds(layer, 1), inside]
                offset = table[:, 8 * source + q : 8 * source + q + 1]
                block = gathered[phase, chunk_rows(c), lanes].astype(f32)
                shaped = (block * table[:, 4:5] + offset) * gain + moved
                act[chunk_rows(c), lanes] = (shaped + shaped * jnp.tanh(shaped)).astype(bf16)
        steps(i)

    def close(layer, halves, steps, i):
        c = inner_first(i)
        for q in halves:
            update = jnp.dot(
                act[chunk_rows(c), :],
                weights[layer * 3 * subs + 2 * subs + q],
                preferred_element_type=f32,
            )
            source = tokens if layer == 0 else out
            lanes = pl.ds(q * qc, qc)
            out[chunk_rows(c), lanes] = (source[chunk_rows(c), lanes].astype(f32) + update).astype(bf16)
        if layer + 1 < layers:
            share_stream(layer + 1, c, out[chunk_rows(c), :].astype(f32))
        steps(i)

    def need(m):
        return (m // 2 + 1) * span

    def part_of(steps):
        return steps * span // 6

    marks = ((6, 7, 8, 9, 13, 14, 15, 16, 18, 20, 20, 22), (28, 28, 28, 30, 32, 33, 35, 36, 36, 36, 36, 36))

    for layer in range(layers):
        first = layer * 3 * subs
        phase = layer * (1 + subs)
        goals = iter([part_of(mark) for mark in marks[layer]])
        loop(functools.partial(arrive, phase, share(next(goals))))
        if layer == 0:
            landed(norms.at[:, pl.ds(0, tp - 1)], n_recv)
        for q in range(subs):
            advance(max(need(first + 2 * q + 1), next(goals)))
            weight_wait(first + 2 * q)
            weight_wait(first + 2 * q + 1)
            loop(functools.partial(gated, layer, q, share(next(goals))))
            forward = phase + q if layer and q else None
            loop(functools.partial(mixed, layer, q, forward, share(next(goals))))
            if q < subs - 1 and layer == 0:
                loop(functools.partial(arrive, phase + 1 + q, share(next(goals))))
        last = first + 2 * subs
        advance(next(goals))
        loop(functools.partial(activate, layer, share(next(goals))))
        advance(max(need(last + subs - 1), next(goals)))
        if layer + 1 < layers:
            for q in range(subs):
                weight_wait(last + q)
            loop(functools.partial(close, layer, range(subs), share(next(goals))))
        else:
            for q in range(subs):
                weight_wait(last + q)
                loop(functools.partial(close, layer, (q,), share(next(goals))))

    for place in range(n):

        @pl.when(sp == place)
        def _():
            if place < n - 1:
                landed(weights.at[:, pl.ds(0, (place + 1) * part), :], z_send.at[0])
                landed(glu.at[:, pl.ds(0, HALO), :], h_send.at[0])
            if place > 0:
                landed(weights.at[:, pl.ds(0, (n - place) * part), :], z_send.at[1])
                landed(glu.at[:, pl.ds(0, HALO), :], h_send.at[1])

    for off in range(1, groups):
        landed(weights.at[:, pl.ds(0, hops * part), :], y_send.at[off - 1])
    landed(gathered.at[:, :, pl.ds(0, (tp - 1) * cols)], x_send)
    landed(stats.at[:, :, pl.ds(0, tp - 1)], s_send)
    landed(norms.at[:, pl.ds(0, tp - 1)], n_send)


def solution(mesh):
    groups, n, tp = mesh.shape["grp"], mesh.shape["sp"], mesh.shape["tp"]

    def shards(tokens, norm_gain, w_value, w_gate, taps, ln_gain, ln_shift, w_out):
        layers, depth, cols = w_value.shape
        count = tokens.shape[0]
        chunks = 3
        subs = 2 if cols % (2 * LANES) == 0 else 1
        pieces = layers * 3 * subs
        taps = jnp.transpose(taps, (1, 0, 2))
        rows = count // chunks
        vmem = pl.BlockSpec(memory_space=pltpu.VMEM)
        hbm = pl.BlockSpec(memory_space=pltpu.HBM)
        dma = pltpu.SemaphoreType.DMA
        return pl.pallas_call(
            functools.partial(body, (groups, n, tp, chunks, subs)),
            out_shape=pltpu.VMEM((count, cols), jnp.bfloat16),
            in_specs=[hbm] * 8,
            out_specs=vmem,
            scratch_shapes=[
                pltpu.VMEM((count, cols), jnp.bfloat16),
                pltpu.VMEM(norm_gain.shape, jnp.float32),
                pltpu.VMEM(taps.shape, jnp.float32),
                pltpu.VMEM((pieces, depth * n, cols // subs), jnp.bfloat16),
                pltpu.VMEM((2 * layers, count, cols * tp), jnp.bfloat16),
                pltpu.VMEM((layers, count + 2 * HALO, cols), jnp.bfloat16),
                pltpu.VMEM((count, cols // subs), jnp.float32),
                pltpu.VMEM((count, cols * tp), jnp.bfloat16),
                pltpu.VMEM((count, LANES), jnp.float32),
                pltpu.VMEM((2 * layers, chunks, tp, 8, rows), jnp.float32),
                pltpu.VMEM((2, tp, layers, cols), jnp.float32),
                dma((6,)),
                dma((2,)),
                dma((pieces, n - 1)),
                dma((groups - 1,)),
                dma((pieces, groups - 1)),
                dma,
                dma((layers * (1 + subs), chunks, tp // 2)),
                dma,
                dma((2 * layers, chunks)),
                dma((2,)),
                dma((layers, subs, 2)),
                dma,
                dma,
            ],
            compiler_params=pltpu.CompilerParams(
                collective_id=0, has_side_effects=True, vmem_limit_bytes=56 * 1024 * 1024
            ),
        )(tokens, norm_gain, w_value, w_gate, taps, ln_gain, ln_shift, w_out)

    return jax.shard_map(
        shards,
        mesh=mesh,
        in_specs=(
            P(("grp", "sp"), "tp"),
            P(),
            P(None, "sp", "tp"),
            P(None, "sp", "tp"),
            P(None, None, "tp"),
            P(None, "tp"),
            P(None, "tp"),
            P(None, "sp", "tp"),
        ),
        out_specs=P(("grp", "sp"), "tp"),
        check_vma=False,
    )
```

```python
import functools

import jax
import jax.numpy as jnp
from jax import lax
from jax.experimental import pallas as pl
from jax.experimental.pallas import tpu as pltpu
from jax.sharding import PartitionSpec as P

MESH = pl.DeviceIdType.MESH
HALO = 16
LANES = 128
BLOCK = 64


def body(
    sizes,
    tokens_in,
    gain_in,
    w_value,
    w_gate,
    taps_in,
    ln_gain,
    ln_shift,
    w_out,
    out,
    tokens,
    norm_gain,
    taps,
    weights,
    gathered,
    glu,
    conv,
    act,
    sums,
    stats,
    norms,
    load_sem,
    z_send,
    z_recv,
    y_send,
    y_recv,
    x_send,
    x_recv,
    s_send,
    s_recv,
    h_send,
    h_recv,
    n_send,
    n_recv,
):
    groups, n, tp, chunks, subs = sizes
    chips = tp // 2
    grp, sp, me = lax.axis_index("grp"), lax.axis_index("sp"), lax.axis_index("tp")
    chip, core = me // 2, me % 2
    partner = chip * 2 + 1 - core
    layers, depth, cols = w_value.shape
    kernel = taps_in.shape[0]
    half = (kernel - 1) // 2
    count = tokens_in.shape[0]
    rows = count // chunks
    width = cols * tp
    hops = n - 1
    f32, bf16 = jnp.float32, jnp.bfloat16

    def aligned(value, unit):
        return pl.multiple_of(value, unit)

    barrier = pltpu.get_barrier_semaphore()
    for off in range(1, tp):
        pl.semaphore_signal(
            barrier, inc=1, device_id={"tp": (me + off) % tp}, device_id_type=MESH
        )
    for off in range(1, groups):
        pl.semaphore_signal(
            barrier, inc=1, device_id={"grp": (grp + off) % groups}, device_id_type=MESH
        )

    @pl.when(sp > 0)
    def _():
        pl.semaphore_signal(barrier, inc=1, device_id={"sp": sp - 1}, device_id_type=MESH)

    @pl.when(sp < n - 1)
    def _():
        pl.semaphore_signal(barrier, inc=1, device_id={"sp": sp + 1}, device_id_type=MESH)

    qc = cols // subs
    total = layers * 3 * subs
    part = depth // groups
    span = 2 * hops

    def own_load(m):
        layer, j = m // (3 * subs), m % (3 * subs)
        if j < 2 * subs:
            source, q = (w_value, w_gate)[j % 2], j // 2
        else:
            source, q = w_out, j - 2 * subs
        return pltpu.make_async_copy(
            source.at[layer, :, pl.ds(q * qc, qc)],
            weights.at[m, pl.ds(aligned(sp * depth, 16), depth), :],
            load_sem.at[0 if m < 2 else 1],
        )

    tokens_load = pltpu.make_async_copy(tokens_in, tokens, load_sem.at[2])
    gain_load = pltpu.make_async_copy(gain_in, norm_gain, load_sem.at[3])
    taps_load = pltpu.make_async_copy(taps_in, taps, load_sem.at[4])
    own_load(0).start()
    own_load(1).start()
    tokens_load.start()
    gain_load.start()

    def piece(block, m, quarter):
        return weights.at[m, pl.ds(aligned(block * depth + quarter * part, 16), part), :]

    def z_copy(way, m, block):
        ref = piece(block, m, grp)
        return pltpu.make_async_remote_copy(
            src_ref=ref,
            dst_ref=ref,
            send_sem=z_send.at[way],
            recv_sem=z_recv.at[m, block - way],
            device_id={"sp": sp + 1 if way == 0 else sp - 1},
            device_id_type=MESH,
        )

    def y_copy(m, block, off, quarter):
        ref = piece(block, m, quarter)
        return pltpu.make_async_remote_copy(
            src_ref=ref,
            dst_ref=ref,
            send_sem=y_send.at[off - 1],
            recv_sem=y_recv.at[m, off - 1],
            device_id={"grp": (grp + off) % groups},
            device_id_type=MESH,
        )

    steps_in_all = total * hops
    below, above = sp, n - 1 - sp
    early = (0 * above, 0 * below)

    def receive(way, k):
        m, r = 2 * (k // span) + k % 2, (k % span) // 2
        sources = below if way == 0 else above
        onward = above > 0 if way == 0 else below > 0

        @pl.when(r < sources)
        def _():
            block = sp - (r + 1) if way == 0 else sp + (r + 1)
            z_copy(way, m, block).wait_recv()

            @pl.when(onward)
            def _():
                z_copy(way, m, block).start()

            for off in range(1, groups):
                y_copy(m, block, off, grp).start()

        @pl.when(jnp.logical_and(jnp.logical_and(r == sources, onward), m + 2 < total))
        def _():
            z_copy(way, m + 2, sp).start()

    def weight_prelude():
        for way in range(2):
            lax.fori_loop(0, early[way], lambda k, c: (receive(way, k), c)[1], 0)

    def weight_step(k):
        for way in range(2):

            @pl.when(k + early[way] < steps_in_all)
            def _():
                receive(way, k + early[way])

    def weight_steps(low, high):
        lax.fori_loop(low, high, lambda k, c: (weight_step(k), c)[1], 0)

    def landed(ref, sem):
        pltpu.make_async_copy(ref, ref, sem).wait()

    def weight_wait(m):
        for off in range(1, groups):
            landed(weights.at[m, pl.ds(0, hops * part), :], y_recv.at[m, off - 1])

    def chunk_rows(c):
        return pl.ds(aligned(c * rows, rows), rows)

    def x_lanes(phase, source):
        sub = phase % (1 + subs)
        if sub == 0:
            return pl.ds(aligned(source * cols, LANES), cols)
        return pl.ds(aligned(source * cols + (sub - 1) * qc, LANES), qc)

    def x_copy(phase, c, source, slot, target):
        layer, sub = phase // (1 + subs), phase % (1 + subs)
        ref = gathered.at[2 * layer + min(sub, 1), chunk_rows(c), x_lanes(phase, source)]
        return pltpu.make_async_remote_copy(
            src_ref=ref,
            dst_ref=ref,
            send_sem=x_send,
            recv_sem=x_recv.at[phase, c, slot],
            device_id={"tp": target},
            device_id_type=MESH,
        )

    def x_own(phase, c):
        for off in range(1, chips):
            x_copy(phase, c, me, off, ((chip + off) % chips) * 2 + core).start()
        x_copy(phase, c, me, 0, partner).start()

    def x_forward(phase, c):
        for off in range(1, chips):
            source = ((chip + chips - off) % chips) * 2 + core
            x_copy(phase, c, source, off, partner).wait_recv()
            x_copy(phase, c, source, 0, partner).start()

    def x_wait(phase, c):
        ref = gathered.at[0, pl.ds(0, rows), pl.ds(0, chips * (cols if phase % (1 + subs) == 0 else qc))]
        landed(ref, x_recv.at[phase, c, 0])

    def s_copy(phase, c, source, target):
        ref = stats.at[phase, c, source]
        return pltpu.make_async_remote_copy(
            src_ref=ref,
            dst_ref=ref,
            send_sem=s_send,
            recv_sem=s_recv.at[phase, c],
            device_id={"tp": target},
            device_id_type=MESH,
        )

    def s_share(phase, c, values):
        stats[phase, c, me] = values.T[:8]
        for off in range(1, tp):
            s_copy(phase, c, me, (me + off) % tp).start()

    def s_wait(phase, c):
        landed(stats.at[phase, c, pl.ds(0, tp - 1)], s_recv.at[phase, c])

    def s_total(phase, c):
        total = stats[phase, c, 0]
        for source in range(1, tp):
            total = total + stats[phase, c, source]
        return total

    def columns(rows_of_8):
        block = jnp.concatenate(rows_of_8, axis=0)
        return jnp.concatenate([block] * (LANES // block.shape[0]), axis=0).T

    def n_load(which):
        source = (ln_gain, ln_shift)[which]
        return pltpu.make_async_copy(source, norms.at[which, me], load_sem.at[5])

    def n_copy(which, target):
        return pltpu.make_async_remote_copy(
            src_ref=(ln_gain, ln_shift)[which],
            dst_ref=norms.at[which, me],
            send_sem=n_send,
            recv_sem=n_recv,
            device_id={"tp": target},
            device_id_type=MESH,
        )

    def h_copy(layer, q, way):
        if way == 0:
            source, target, device = count, 0, sp + 1
        else:
            source, target, device = HALO, HALO + count, sp - 1
        lanes = pl.ds(q * qc, qc)
        return pltpu.make_async_remote_copy(
            src_ref=glu.at[layer, pl.ds(source, HALO), lanes],
            dst_ref=glu.at[layer, pl.ds(target, HALO), lanes],
            send_sem=h_send.at[way],
            recv_sem=h_recv.at[layer, q, way],
            device_id={"sp": device},
            device_id_type=MESH,
        )

    mine = pl.ds(aligned(me * cols, LANES), cols)
    lane = lax.broadcasted_iota(jnp.int32, (rows, LANES), 1)

    def share_stream(layer, c, wide):
        gain = norm_gain[pl.ds(layer, 1), mine]
        gathered[2 * layer, chunk_rows(c), mine] = (wide * gain).astype(bf16)
        x_own(layer * (1 + subs), c)
        square = jnp.sum(wide * wide, axis=1, keepdims=True)
        s_share(2 * layer, c, jnp.where(lane == 0, square, 0.0))

    def loop(function, low=0, high=chunks):
        lax.fori_loop(low, high, lambda i, c: (function(i), c)[1], 0)

    def inner_first(i):
        return (1 + 2 * i) % chunks

    def conv_order(layer, i):
        return (1 + (1 if layer else 2) * i) % chunks

    def ends_first(i):
        return (2 * i) % chunks

    for layer in range(layers):

        @pl.when(sp == 0)
        def _():
            glu[layer, pl.ds(0, HALO), :] = jnp.zeros((HALO, cols), bf16)

        @pl.when(sp == n - 1)
        def _():
            glu[layer, pl.ds(HALO + count, HALO), :] = jnp.zeros((HALO, cols), bf16)

    landed(weights.at[pl.ds(0, 2), pl.ds(0, depth), :], load_sem.at[0])
    pl.semaphore_wait(
        barrier,
        tp - 1 + groups - 1 + (sp > 0).astype(jnp.int32) + (sp < n - 1).astype(jnp.int32),
    )
    for m in range(2):

        @pl.when(sp < n - 1)
        def _():
            z_copy(0, m, sp).start()

        @pl.when(sp > 0)
        def _():
            z_copy(1, m, sp).start()

    for m in range(2, total):
        own_load(m).start()
    taps_load.start()
    for which in range(2):
        n_load(which).start()
    tokens_load.wait()
    gain_load.wait()
    loop(lambda c: share_stream(0, c, tokens[chunk_rows(c), :].astype(f32)))
    for which in range(2):
        for off in range(1, tp):
            n_copy(which, (me + off) % tp).start()
    landed(weights.at[pl.ds(2, total - 2), pl.ds(0, depth), :], load_sem.at[1])
    taps_load.wait()
    landed(norms.at[:, 0], load_sem.at[5])

    weight_prelude()
    done = [0]

    def share(goal):
        low = done[0]
        high = max(low, min(goal, total * hops))
        done[0] = high
        return lambda i: weight_steps(
            low + (high - low) * i // chunks, low + (high - low) * (i + 1) // chunks
        )

    def advance(goal):
        low = done[0]
        high = max(low, min(goal, total * hops))
        done[0] = high
        weight_steps(low, high)

    def gated(layer, q, steps, i):
        c = inner_first(i) if layer and q == 0 else ends_first(i)
        if q == 0:
            s_wait(2 * layer, c)
        scale = lax.rsqrt(columns([s_total(2 * layer, c)])[:, :1] / width + 1e-06)
        block = gathered[2 * layer, chunk_rows(c), :]
        first = layer * 3 * subs + 2 * q
        value = jnp.dot(block, weights[first], preferred_element_type=f32) * scale
        gate = jnp.dot(block, weights[first + 1], preferred_element_type=f32) * (0.5 * scale)
        glu[layer, pl.ds(aligned(HALO + c * rows, HALO), rows), pl.ds(q * qc, qc)] = (
            value * (0.5 + 0.5 * jnp.tanh(gate))
        ).astype(bf16)

        @pl.when(jnp.logical_and(c == 0, sp > 0))
        def _():
            h_copy(layer, q, 1).start()

        @pl.when(jnp.logical_and(c == chunks - 1, sp < n - 1))
        def _():
            h_copy(layer, q, 0).start()

        if steps is not None:
            steps(i)

    shift = HALO - half
    groups_of_8 = (kernel + shift + 7) // 8
    window = BLOCK + 8 * groups_of_8

    def convolve(layer, q, c):
        lane_blocks = qc // LANES

        def block(i, carry):
            base = aligned(c * rows + (i // lane_blocks) * BLOCK, BLOCK)
            inside = aligned((i % lane_blocks) * LANES, LANES)
            lanes = pl.ds(aligned(q * qc + inside, LANES), LANES)
            values = glu[layer, pl.ds(base, window), lanes].astype(f32)
            total = None
            for j in range(8):
                partial = None
                for g in range(groups_of_8):
                    tap = 8 * g + j - shift
                    if tap < 0 or tap >= kernel:
                        continue
                    term = taps[tap, pl.ds(layer, 1), lanes] * values[8 * g : 8 * g + BLOCK + 8]
                    partial = term if partial is None else partial + term
                piece_j = partial[j : j + BLOCK]
                total = piece_j if total is None else total + piece_j
            conv[pl.ds(base, BLOCK), pl.ds(inside, LANES)] = total
            return carry

        lax.fori_loop(0, rows // BLOCK * lane_blocks, block, 0)

    def mixed(layer, q, forward, steps, i):
        c = conv_order(layer, i)

        @pl.when(jnp.logical_and(c == 0, sp > 0))
        def _():
            h_copy(layer, q, 0).wait_recv()

        @pl.when(jnp.logical_and(c == chunks - 1, sp < n - 1))
        def _():
            h_copy(layer, q, 1).wait_recv()

        convolve(layer, q, c)
        whole = conv[chunk_rows(c), :]
        row_sum = jnp.sum(whole, axis=1, keepdims=True)
        lanes = pl.ds(aligned(me * cols + q * qc, LANES), qc)
        gathered[2 * layer + 1, chunk_rows(c), lanes] = (whole - row_sum / qc).astype(bf16)
        x_own(layer * (1 + subs) + 1 + q, c)
        square = jnp.sum(whole * whole, axis=1, keepdims=True)
        both = jnp.where(lane == q, row_sum, jnp.where(lane == 4, square, 0.0))
        if q > 0:
            both = both + sums[chunk_rows(c), :]
        if q < subs - 1:
            sums[chunk_rows(c), :] = both
        else:
            s_share(2 * layer + 1, c, both)
        if forward is not None:
            x_forward(forward, c)
        steps(i)

    def arrive(phase, steps, i):
        c = i if phase == 0 else inner_first(i)
        if steps is not None:
            steps(i)
        x_forward(phase, c)
        x_wait(phase, c)

    sublane = lax.broadcasted_iota(jnp.int32, (8, rows), 0)

    def activate(layer, steps, i):
        c = conv_order(layer, i)
        phase = 2 * layer + 1
        x_forward(layer * (1 + subs) + subs, c)
        s_wait(phase, c)
        for q in range(0 if layer else subs - 1, subs):
            x_wait(layer * (1 + subs) + 1 + q, c)
        total = s_total(phase, c)
        mean = total[0:1]
        for q in range(1, subs):
            mean = mean + total[q : q + 1]
        mean = mean / width
        inverse = lax.rsqrt(total[4:5] / width - mean * mean + 1e-05)
        offsets = [
            jnp.where(sublane == 4, inverse, (stats[phase, c, source] / qc - mean) * inverse)
            for source in range(tp)
        ]
        table = columns(offsets)
        for source in range(tp):
            for q in range(subs):
                lanes = pl.ds(source * cols + q * qc, qc)
                inside = pl.ds(q * qc, qc)
                gain = 0.5 * norms[0, source, pl.ds(layer, 1), inside]
                moved = 0.5 * norms[1, source, pl.ds(layer, 1), inside]
                offset = table[:, 8 * source + q : 8 * source + q + 1]
                block = gathered[phase, chunk_rows(c), lanes].astype(f32)
                shaped = (block * table[:, 4:5] + offset) * gain + moved
                act[chunk_rows(c), lanes] = (shaped + shaped * jnp.tanh(shaped)).astype(bf16)
        steps(i)

    def close(layer, halves, steps, i):
        c = inner_first(i)
        for q in halves:
            update = jnp.dot(
                act[chunk_rows(c), :],
                weights[layer * 3 * subs + 2 * subs + q],
                preferred_element_type=f32,
            )
            source = tokens if layer == 0 else out
            lanes = pl.ds(q * qc, qc)
            out[chunk_rows(c), lanes] = (source[chunk_rows(c), lanes].astype(f32) + update).astype(bf16)
        if layer + 1 < layers:
            share_stream(layer + 1, c, out[chunk_rows(c), :].astype(f32))
        steps(i)

    def need(m):
        return (m // 2 + 1) * span

    def part_of(steps):
        return steps * span // 6

    marks = ((6, 8, 9, 10, 13, 14, 15, 17, 18, 20, 20, 22), (24, 26, 26, 27, 28, 29, 32, 33, 35, 36, 36, 36, 36, 36))

    for layer in range(layers):
        first = layer * 3 * subs
        phase = layer * (1 + subs)
        goals = iter([part_of(mark) for mark in marks[layer]])
        if layer == 0:
            loop(functools.partial(arrive, phase, share(next(goals))))
            landed(norms.at[:, pl.ds(0, tp - 1)], n_recv)
        else:
            for i in range(chunks - 1):
                advance(next(goals))
                arrive(phase, None, i)
        for q in range(subs):
            advance(max(need(first + 2 * q + 1), next(goals)))
            weight_wait(first + 2 * q)
            weight_wait(first + 2 * q + 1)
            if layer and q == 0:
                loop(functools.partial(gated, layer, q, None), 0, chunks - 1)
                advance(next(goals))
                arrive(phase, None, chunks - 1)
                gated(layer, q, None, chunks - 1)
                advance(next(goals))
            else:
                loop(functools.partial(gated, layer, q, share(next(goals))))
            forward = phase + q if layer and q else None
            loop(functools.partial(mixed, layer, q, forward, share(next(goals))))
            if q < subs - 1 and layer == 0:
                loop(functools.partial(arrive, phase + 1 + q, share(next(goals))))
        last = first + 2 * subs
        advance(next(goals))
        loop(functools.partial(activate, layer, share(next(goals))))
        advance(max(need(last + subs - 1), next(goals)))
        if layer + 1 < layers:
            for q in range(subs):
                weight_wait(last + q)
            loop(functools.partial(close, layer, range(subs), share(next(goals))))
        else:
            for q in range(subs):
                weight_wait(last + q)
                loop(functools.partial(close, layer, (q,), share(next(goals))))

    for place in range(n):

        @pl.when(sp == place)
        def _():
            if place < n - 1:
                landed(weights.at[:, pl.ds(0, (place + 1) * part), :], z_send.at[0])
                landed(glu.at[:, pl.ds(0, HALO), :], h_send.at[0])
            if place > 0:
                landed(weights.at[:, pl.ds(0, (n - place) * part), :], z_send.at[1])
                landed(glu.at[:, pl.ds(0, HALO), :], h_send.at[1])

    for off in range(1, groups):
        landed(weights.at[:, pl.ds(0, hops * part), :], y_send.at[off - 1])
    landed(gathered.at[:, :, pl.ds(0, (tp - 1) * cols)], x_send)
    landed(stats.at[:, :, pl.ds(0, tp - 1)], s_send)
    landed(norms.at[:, pl.ds(0, tp - 1)], n_send)


def solution(mesh):
    groups, n, tp = mesh.shape["grp"], mesh.shape["sp"], mesh.shape["tp"]

    def shards(tokens, norm_gain, w_value, w_gate, taps, ln_gain, ln_shift, w_out):
        layers, depth, cols = w_value.shape
        count = tokens.shape[0]
        chunks = 3
        subs = 2 if cols % (2 * LANES) == 0 else 1
        pieces = layers * 3 * subs
        taps = jnp.transpose(taps, (1, 0, 2))
        rows = count // chunks
        vmem = pl.BlockSpec(memory_space=pltpu.VMEM)
        hbm = pl.BlockSpec(memory_space=pltpu.HBM)
        dma = pltpu.SemaphoreType.DMA
        return pl.pallas_call(
            functools.partial(body, (groups, n, tp, chunks, subs)),
            out_shape=pltpu.VMEM((count, cols), jnp.bfloat16),
            in_specs=[hbm] * 8,
            out_specs=vmem,
            scratch_shapes=[
                pltpu.VMEM((count, cols), jnp.bfloat16),
                pltpu.VMEM(norm_gain.shape, jnp.float32),
                pltpu.VMEM(taps.shape, jnp.float32),
                pltpu.VMEM((pieces, depth * n, cols // subs), jnp.bfloat16),
                pltpu.VMEM((2 * layers, count, cols * tp), jnp.bfloat16),
                pltpu.VMEM((layers, count + 2 * HALO, cols), jnp.bfloat16),
                pltpu.VMEM((count, cols // subs), jnp.float32),
                pltpu.VMEM((count, cols * tp), jnp.bfloat16),
                pltpu.VMEM((count, LANES), jnp.float32),
                pltpu.VMEM((2 * layers, chunks, tp, 8, rows), jnp.float32),
                pltpu.VMEM((2, tp, layers, cols), jnp.float32),
                dma((6,)),
                dma((2,)),
                dma((pieces, n - 1)),
                dma((groups - 1,)),
                dma((pieces, groups - 1)),
                dma,
                dma((layers * (1 + subs), chunks, tp // 2)),
                dma,
                dma((2 * layers, chunks)),
                dma((2,)),
                dma((layers, subs, 2)),
                dma,
                dma,
            ],
            compiler_params=pltpu.CompilerParams(
                collective_id=0, has_side_effects=True, vmem_limit_bytes=56 * 1024 * 1024
            ),
        )(tokens, norm_gain, w_value, w_gate, taps, ln_gain, ln_shift, w_out)

    return jax.shard_map(
        shards,
        mesh=mesh,
        in_specs=(
            P(("grp", "sp"), "tp"),
            P(),
            P(None, "sp", "tp"),
            P(None, "sp", "tp"),
            P(None, None, "tp"),
            P(None, "tp"),
            P(None, "tp"),
            P(None, "sp", "tp"),
        ),
        out_specs=P(("grp", "sp"), "tp"),
        check_vma=False,
    )
```

```python
import functools

import jax
import jax.numpy as jnp
from jax import lax
from jax.experimental import pallas as pl
from jax.experimental.pallas import tpu as pltpu
from jax.sharding import PartitionSpec as P

MESH = pl.DeviceIdType.MESH
HALO = 16
LANES = 128
BLOCK = 64


def body(
    sizes,
    tokens_in,
    gain_in,
    w_value,
    w_gate,
    taps_in,
    ln_gain,
    ln_shift,
    w_out,
    out,
    tokens,
    norm_gain,
    taps,
    weights,
    gathered,
    glu,
    conv,
    act,
    sums,
    stats,
    norms,
    load_sem,
    z_send,
    z_recv,
    y_send,
    y_recv,
    x_send,
    x_recv,
    s_send,
    s_recv,
    h_send,
    h_recv,
    n_send,
    n_recv,
):
    groups, n, tp, chunks, subs = sizes
    chips = tp // 2
    grp, sp, me = lax.axis_index("grp"), lax.axis_index("sp"), lax.axis_index("tp")
    chip, core = me // 2, me % 2
    partner = chip * 2 + 1 - core
    layers, depth, cols = w_value.shape
    kernel = taps_in.shape[0]
    half = (kernel - 1) // 2
    count = tokens_in.shape[0]
    rows = count // chunks
    width = cols * tp
    hops = n - 1
    f32, bf16 = jnp.float32, jnp.bfloat16

    def aligned(value, unit):
        return pl.multiple_of(value, unit)

    barrier = pltpu.get_barrier_semaphore()
    for off in range(1, tp):
        pl.semaphore_signal(
            barrier, inc=1, device_id={"tp": (me + off) % tp}, device_id_type=MESH
        )
    for off in range(1, groups):
        pl.semaphore_signal(
            barrier, inc=1, device_id={"grp": (grp + off) % groups}, device_id_type=MESH
        )

    @pl.when(sp > 0)
    def _():
        pl.semaphore_signal(barrier, inc=1, device_id={"sp": sp - 1}, device_id_type=MESH)

    @pl.when(sp < n - 1)
    def _():
        pl.semaphore_signal(barrier, inc=1, device_id={"sp": sp + 1}, device_id_type=MESH)

    qc = cols // subs
    total = layers * 3 * subs
    part = depth // groups
    span = 2 * hops

    def own_load(m):
        layer, j = m // (3 * subs), m % (3 * subs)
        if j < 2 * subs:
            source, q = (w_value, w_gate)[j % 2], j // 2
        else:
            source, q = w_out, j - 2 * subs
        return pltpu.make_async_copy(
            source.at[layer, :, pl.ds(q * qc, qc)],
            weights.at[m, pl.ds(aligned(sp * depth, 16), depth), :],
            load_sem.at[0 if m < 2 else 1],
        )

    tokens_load = pltpu.make_async_copy(tokens_in, tokens, load_sem.at[2])
    gain_load = pltpu.make_async_copy(gain_in, norm_gain, load_sem.at[3])
    taps_load = pltpu.make_async_copy(taps_in, taps, load_sem.at[4])
    own_load(0).start()
    own_load(1).start()
    tokens_load.start()
    gain_load.start()

    def piece(block, m, quarter):
        return weights.at[m, pl.ds(aligned(block * depth + quarter * part, 16), part), :]

    def z_copy(way, m, block):
        ref = piece(block, m, grp)
        return pltpu.make_async_remote_copy(
            src_ref=ref,
            dst_ref=ref,
            send_sem=z_send.at[way],
            recv_sem=z_recv.at[m, block - way],
            device_id={"sp": sp + 1 if way == 0 else sp - 1},
            device_id_type=MESH,
        )

    def y_copy(m, block, off, quarter):
        ref = piece(block, m, quarter)
        return pltpu.make_async_remote_copy(
            src_ref=ref,
            dst_ref=ref,
            send_sem=y_send.at[off - 1],
            recv_sem=y_recv.at[m, off - 1],
            device_id={"grp": (grp + off) % groups},
            device_id_type=MESH,
        )

    steps_in_all = total * hops
    below, above = sp, n - 1 - sp
    early = (0 * above, 0 * below)

    def receive(way, k):
        m, r = 2 * (k // span) + k % 2, (k % span) // 2
        sources = below if way == 0 else above
        onward = above > 0 if way == 0 else below > 0

        @pl.when(r < sources)
        def _():
            block = sp - (r + 1) if way == 0 else sp + (r + 1)
            z_copy(way, m, block).wait_recv()

            @pl.when(onward)
            def _():
                z_copy(way, m, block).start()

            for off in range(1, groups):
                y_copy(m, block, off, grp).start()

        @pl.when(jnp.logical_and(jnp.logical_and(r == sources, onward), m + 2 < total))
        def _():
            z_copy(way, m + 2, sp).start()

    def weight_prelude():
        for way in range(2):
            lax.fori_loop(0, early[way], lambda k, c: (receive(way, k), c)[1], 0)

    def weight_step(k):
        for way in range(2):

            @pl.when(k + early[way] < steps_in_all)
            def _():
                receive(way, k + early[way])

    def weight_steps(low, high):
        lax.fori_loop(low, high, lambda k, c: (weight_step(k), c)[1], 0)

    def landed(ref, sem):
        pltpu.make_async_copy(ref, ref, sem).wait()

    def weight_wait(m):
        for off in range(1, groups):
            landed(weights.at[m, pl.ds(0, hops * part), :], y_recv.at[m, off - 1])

    def chunk_rows(c):
        return pl.ds(aligned(c * rows, rows), rows)

    def x_lanes(phase, source):
        sub = phase % (1 + subs)
        if sub == 0:
            return pl.ds(aligned(source * cols, LANES), cols)
        return pl.ds(aligned(source * cols + (sub - 1) * qc, LANES), qc)

    def x_copy(phase, c, source, slot, target):
        layer, sub = phase // (1 + subs), phase % (1 + subs)
        ref = gathered.at[2 * layer + min(sub, 1), chunk_rows(c), x_lanes(phase, source)]
        return pltpu.make_async_remote_copy(
            src_ref=ref,
            dst_ref=ref,
            send_sem=x_send,
            recv_sem=x_recv.at[phase, c, slot],
            device_id={"tp": target},
            device_id_type=MESH,
        )

    def x_own(phase, c):
        for off in range(1, chips):
            x_copy(phase, c, me, off, ((chip + off) % chips) * 2 + core).start()
        x_copy(phase, c, me, 0, partner).start()

    def x_forward(phase, c):
        for off in range(1, chips):
            source = ((chip + chips - off) % chips) * 2 + core
            x_copy(phase, c, source, off, partner).wait_recv()
            x_copy(phase, c, source, 0, partner).start()

    def x_wait(phase, c):
        ref = gathered.at[0, pl.ds(0, rows), pl.ds(0, chips * (cols if phase % (1 + subs) == 0 else qc))]
        landed(ref, x_recv.at[phase, c, 0])

    def s_copy(phase, c, source, target):
        ref = stats.at[phase, c, source]
        return pltpu.make_async_remote_copy(
            src_ref=ref,
            dst_ref=ref,
            send_sem=s_send,
            recv_sem=s_recv.at[phase, c],
            device_id={"tp": target},
            device_id_type=MESH,
        )

    def s_share(phase, c, values):
        stats[phase, c, me] = values.T[:8]
        for off in range(1, tp):
            s_copy(phase, c, me, (me + off) % tp).start()

    def s_wait(phase, c):
        landed(stats.at[phase, c, pl.ds(0, tp - 1)], s_recv.at[phase, c])

    def s_total(phase, c):
        total = stats[phase, c, 0]
        for source in range(1, tp):
            total = total + stats[phase, c, source]
        return total

    def columns(rows_of_8):
        block = jnp.concatenate(rows_of_8, axis=0)
        return jnp.concatenate([block] * (LANES // block.shape[0]), axis=0).T

    def n_load(which):
        source = (ln_gain, ln_shift)[which]
        return pltpu.make_async_copy(source, norms.at[which, me], load_sem.at[5])

    def n_copy(which, target):
        return pltpu.make_async_remote_copy(
            src_ref=(ln_gain, ln_shift)[which],
            dst_ref=norms.at[which, me],
            send_sem=n_send,
            recv_sem=n_recv,
            device_id={"tp": target},
            device_id_type=MESH,
        )

    def h_copy(layer, q, way):
        if way == 0:
            source, target, device = count, 0, sp + 1
        else:
            source, target, device = HALO, HALO + count, sp - 1
        lanes = pl.ds(q * qc, qc)
        return pltpu.make_async_remote_copy(
            src_ref=glu.at[layer, pl.ds(source, HALO), lanes],
            dst_ref=glu.at[layer, pl.ds(target, HALO), lanes],
            send_sem=h_send.at[way],
            recv_sem=h_recv.at[layer, q, way],
            device_id={"sp": device},
            device_id_type=MESH,
        )

    mine = pl.ds(aligned(me * cols, LANES), cols)
    lane = lax.broadcasted_iota(jnp.int32, (rows, LANES), 1)

    def share_stream(layer, c, wide):
        gain = norm_gain[pl.ds(layer, 1), mine]
        gathered[2 * layer, chunk_rows(c), mine] = (wide * gain).astype(bf16)
        x_own(layer * (1 + subs), c)
        square = jnp.sum(wide * wide, axis=1, keepdims=True)
        s_share(2 * layer, c, jnp.where(lane == 0, square, 0.0))

    def loop(function, low=0, high=chunks):
        lax.fori_loop(low, high, lambda i, c: (function(i), c)[1], 0)

    def inner_first(i):
        return (1 + 2 * i) % chunks

    def conv_order(layer, i):
        return (1 + (1 if layer else 2) * i) % chunks

    def ends_first(i):
        return (2 * i) % chunks

    for layer in range(layers):

        @pl.when(sp == 0)
        def _():
            glu[layer, pl.ds(0, HALO), :] = jnp.zeros((HALO, cols), bf16)

        @pl.when(sp == n - 1)
        def _():
            glu[layer, pl.ds(HALO + count, HALO), :] = jnp.zeros((HALO, cols), bf16)

    landed(weights.at[pl.ds(0, 2), pl.ds(0, depth), :], load_sem.at[0])
    pl.semaphore_wait(
        barrier,
        tp - 1 + groups - 1 + (sp > 0).astype(jnp.int32) + (sp < n - 1).astype(jnp.int32),
    )
    for m in range(2):

        @pl.when(sp < n - 1)
        def _():
            z_copy(0, m, sp).start()

        @pl.when(sp > 0)
        def _():
            z_copy(1, m, sp).start()

    for m in range(2, total):
        own_load(m).start()
    taps_load.start()
    for which in range(2):
        n_load(which).start()
    tokens_load.wait()
    gain_load.wait()
    loop(lambda c: share_stream(0, c, tokens[chunk_rows(c), :].astype(f32)))
    for which in range(2):
        for off in range(1, tp):
            n_copy(which, (me + off) % tp).start()
    landed(weights.at[pl.ds(2, total - 2), pl.ds(0, depth), :], load_sem.at[1])
    taps_load.wait()
    landed(norms.at[:, 0], load_sem.at[5])

    weight_prelude()
    done = [0]

    def share(goal):
        low = done[0]
        high = max(low, min(goal, total * hops))
        done[0] = high
        return lambda i: weight_steps(
            low + (high - low) * i // chunks, low + (high - low) * (i + 1) // chunks
        )

    def advance(goal):
        low = done[0]
        high = max(low, min(goal, total * hops))
        done[0] = high
        weight_steps(low, high)

    def gated(layer, q, steps, i):
        c = inner_first(i) if layer and q == 0 else ends_first(i)
        if q == 0:
            s_wait(2 * layer, c)
        scale = lax.rsqrt(columns([s_total(2 * layer, c)])[:, :1] / width + 1e-06)
        block = gathered[2 * layer, chunk_rows(c), :]
        first = layer * 3 * subs + 2 * q
        value = jnp.dot(block, weights[first], preferred_element_type=f32) * scale
        gate = jnp.dot(block, weights[first + 1], preferred_element_type=f32) * (0.5 * scale)
        glu[layer, pl.ds(aligned(HALO + c * rows, HALO), rows), pl.ds(q * qc, qc)] = (
            value * (0.5 + 0.5 * jnp.tanh(gate))
        ).astype(bf16)

        @pl.when(jnp.logical_and(c == 0, sp > 0))
        def _():
            h_copy(layer, q, 1).start()

        @pl.when(jnp.logical_and(c == chunks - 1, sp < n - 1))
        def _():
            h_copy(layer, q, 0).start()

        if steps is not None:
            steps(i)

    shift = HALO - half
    groups_of_8 = (kernel + shift + 7) // 8
    window = BLOCK + 8 * groups_of_8

    def convolve(layer, q, c):
        lane_blocks = qc // LANES

        def block(i, carry):
            base = aligned(c * rows + (i // lane_blocks) * BLOCK, BLOCK)
            inside = aligned((i % lane_blocks) * LANES, LANES)
            lanes = pl.ds(aligned(q * qc + inside, LANES), LANES)
            values = glu[layer, pl.ds(base, window), lanes].astype(f32)
            total = None
            for j in range(8):
                partial = None
                for g in range(groups_of_8):
                    tap = 8 * g + j - shift
                    if tap < 0 or tap >= kernel:
                        continue
                    term = taps[tap, pl.ds(layer, 1), lanes] * values[8 * g : 8 * g + BLOCK + 8]
                    partial = term if partial is None else partial + term
                piece_j = partial[j : j + BLOCK]
                total = piece_j if total is None else total + piece_j
            conv[pl.ds(base, BLOCK), pl.ds(inside, LANES)] = total
            return carry

        lax.fori_loop(0, rows // BLOCK * lane_blocks, block, 0)

    def mixed(layer, q, forward, steps, i):
        c = conv_order(layer, i)

        @pl.when(jnp.logical_and(c == 0, sp > 0))
        def _():
            h_copy(layer, q, 0).wait_recv()

        @pl.when(jnp.logical_and(c == chunks - 1, sp < n - 1))
        def _():
            h_copy(layer, q, 1).wait_recv()

        convolve(layer, q, c)
        whole = conv[chunk_rows(c), :]
        row_sum = jnp.sum(whole, axis=1, keepdims=True)
        lanes = pl.ds(aligned(me * cols + q * qc, LANES), qc)
        gathered[2 * layer + 1, chunk_rows(c), lanes] = (whole - row_sum / qc).astype(bf16)
        x_own(layer * (1 + subs) + 1 + q, c)
        square = jnp.sum(whole * whole, axis=1, keepdims=True)
        both = jnp.where(lane == q, row_sum, jnp.where(lane == 4, square, 0.0))
        if q > 0:
            both = both + sums[chunk_rows(c), :]
        if q < subs - 1:
            sums[chunk_rows(c), :] = both
        else:
            s_share(2 * layer + 1, c, both)
        if forward is not None:
            x_forward(forward, c)
        steps(i)

    def arrive(phase, steps, i):
        c = i if phase == 0 else inner_first(i)
        if steps is not None:
            steps(i)
        x_forward(phase, c)
        x_wait(phase, c)

    sublane = lax.broadcasted_iota(jnp.int32, (8, rows), 0)

    def activate(layer, steps, i):
        c = conv_order(layer, i)
        phase = 2 * layer + 1
        x_forward(layer * (1 + subs) + subs, c)
        s_wait(phase, c)
        for q in range(0 if layer else subs - 1, subs):
            x_wait(layer * (1 + subs) + 1 + q, c)
        total = s_total(phase, c)
        mean = total[0:1]
        for q in range(1, subs):
            mean = mean + total[q : q + 1]
        mean = mean / width
        inverse = lax.rsqrt(total[4:5] / width - mean * mean + 1e-05)
        offsets = [
            jnp.where(sublane == 4, inverse, (stats[phase, c, source] / qc - mean) * inverse)
            for source in range(tp)
        ]
        table = columns(offsets)
        for source in range(tp):
            for q in range(subs):
                lanes = pl.ds(source * cols + q * qc, qc)
                inside = pl.ds(q * qc, qc)
                gain = 0.5 * norms[0, source, pl.ds(layer, 1), inside]
                moved = 0.5 * norms[1, source, pl.ds(layer, 1), inside]
                offset = table[:, 8 * source + q : 8 * source + q + 1]
                block = gathered[phase, chunk_rows(c), lanes].astype(f32)
                shaped = (block * table[:, 4:5] + offset) * gain + moved
                act[chunk_rows(c), lanes] = (shaped + shaped * jnp.tanh(shaped)).astype(bf16)
        if steps is not None:
            steps(i)

    def close(layer, halves, steps, i):
        c = inner_first(i) if layer + 1 < layers else conv_order(layer, i)
        for q in halves:
            update = jnp.dot(
                act[chunk_rows(c), :],
                weights[layer * 3 * subs + 2 * subs + q],
                preferred_element_type=f32,
            )
            source = tokens if layer == 0 else out
            lanes = pl.ds(q * qc, qc)
            out[chunk_rows(c), lanes] = (source[chunk_rows(c), lanes].astype(f32) + update).astype(bf16)
        if layer + 1 < layers:
            share_stream(layer + 1, c, out[chunk_rows(c), :].astype(f32))
            steps(i)

    def need(m):
        return (m // 2 + 1) * span

    def part_of(steps):
        return steps * span // 6

    marks = ((6, 8, 9, 10, 13, 14, 15, 17, 18, 20, 20, 22), (24, 26, 26, 27, 28, 29, 32, 33, 35, 36, 36, 36))

    for layer in range(layers):
        first = layer * 3 * subs
        phase = layer * (1 + subs)
        goals = iter([part_of(mark) for mark in marks[layer]])
        if layer == 0:
            loop(functools.partial(arrive, phase, share(next(goals))))
            landed(norms.at[:, pl.ds(0, tp - 1)], n_recv)
        else:
            for i in range(chunks - 1):
                advance(next(goals))
                arrive(phase, None, i)
        for q in range(subs):
            advance(max(need(first + 2 * q + 1), next(goals)))
            weight_wait(first + 2 * q)
            weight_wait(first + 2 * q + 1)
            if layer and q == 0:
                loop(functools.partial(gated, layer, q, None), 0, chunks - 1)
                advance(next(goals))
                arrive(phase, None, chunks - 1)
                gated(layer, q, None, chunks - 1)
                advance(next(goals))
            else:
                loop(functools.partial(gated, layer, q, share(next(goals))))
            forward = phase + q if layer and q else None
            loop(functools.partial(mixed, layer, q, forward, share(next(goals))))
            if q < subs - 1 and layer == 0:
                loop(functools.partial(arrive, phase + 1 + q, share(next(goals))))
        last = first + 2 * subs
        advance(next(goals))
        if layer + 1 < layers:
            loop(functools.partial(activate, layer, share(next(goals))))
            advance(max(need(last + subs - 1), next(goals)))
            for q in range(subs):
                weight_wait(last + q)
            loop(functools.partial(close, layer, range(subs), share(next(goals))))
        else:
            for i in range(chunks - 1):
                activate(layer, None, i)
                advance(next(goals))
            advance(steps_in_all)
            weight_wait(last)
            loop(functools.partial(close, layer, (0,), None), 0, chunks - 1)
            activate(layer, None, chunks - 1)
            close(layer, (0,), None, chunks - 1)
            for q in range(1, subs):
                weight_wait(last + q)
                loop(functools.partial(close, layer, (q,), None))

    for place in range(n):

        @pl.when(sp == place)
        def _():
            if place < n - 1:
                landed(weights.at[:, pl.ds(0, (place + 1) * part), :], z_send.at[0])
                landed(glu.at[:, pl.ds(0, HALO), :], h_send.at[0])
            if place > 0:
                landed(weights.at[:, pl.ds(0, (n - place) * part), :], z_send.at[1])
                landed(glu.at[:, pl.ds(0, HALO), :], h_send.at[1])

    for off in range(1, groups):
        landed(weights.at[:, pl.ds(0, hops * part), :], y_send.at[off - 1])
    landed(gathered.at[:, :, pl.ds(0, (tp - 1) * cols)], x_send)
    landed(stats.at[:, :, pl.ds(0, tp - 1)], s_send)
    landed(norms.at[:, pl.ds(0, tp - 1)], n_send)


def solution(mesh):
    groups, n, tp = mesh.shape["grp"], mesh.shape["sp"], mesh.shape["tp"]

    def shards(tokens, norm_gain, w_value, w_gate, taps, ln_gain, ln_shift, w_out):
        layers, depth, cols = w_value.shape
        count = tokens.shape[0]
        chunks = 3
        subs = 2 if cols % (2 * LANES) == 0 else 1
        pieces = layers * 3 * subs
        taps = jnp.transpose(taps, (1, 0, 2))
        rows = count // chunks
        vmem = pl.BlockSpec(memory_space=pltpu.VMEM)
        hbm = pl.BlockSpec(memory_space=pltpu.HBM)
        dma = pltpu.SemaphoreType.DMA
        return pl.pallas_call(
            functools.partial(body, (groups, n, tp, chunks, subs)),
            out_shape=pltpu.VMEM((count, cols), jnp.bfloat16),
            in_specs=[hbm] * 8,
            out_specs=vmem,
            scratch_shapes=[
                pltpu.VMEM((count, cols), jnp.bfloat16),
                pltpu.VMEM(norm_gain.shape, jnp.float32),
                pltpu.VMEM(taps.shape, jnp.float32),
                pltpu.VMEM((pieces, depth * n, cols // subs), jnp.bfloat16),
                pltpu.VMEM((2 * layers, count, cols * tp), jnp.bfloat16),
                pltpu.VMEM((layers, count + 2 * HALO, cols), jnp.bfloat16),
                pltpu.VMEM((count, cols // subs), jnp.float32),
                pltpu.VMEM((count, cols * tp), jnp.bfloat16),
                pltpu.VMEM((count, LANES), jnp.float32),
                pltpu.VMEM((2 * layers, chunks, tp, 8, rows), jnp.float32),
                pltpu.VMEM((2, tp, layers, cols), jnp.float32),
                dma((6,)),
                dma((2,)),
                dma((pieces, n - 1)),
                dma((groups - 1,)),
                dma((pieces, groups - 1)),
                dma,
                dma((layers * (1 + subs), chunks, tp // 2)),
                dma,
                dma((2 * layers, chunks)),
                dma((2,)),
                dma((layers, subs, 2)),
                dma,
                dma,
            ],
            compiler_params=pltpu.CompilerParams(
                collective_id=0, has_side_effects=True, vmem_limit_bytes=56 * 1024 * 1024
            ),
        )(tokens, norm_gain, w_value, w_gate, taps, ln_gain, ln_shift, w_out)

    return jax.shard_map(
        shards,
        mesh=mesh,
        in_specs=(
            P(("grp", "sp"), "tp"),
            P(),
            P(None, "sp", "tp"),
            P(None, "sp", "tp"),
            P(None, None, "tp"),
            P(None, "tp"),
            P(None, "tp"),
            P(None, "sp", "tp"),
        ),
        out_specs=P(("grp", "sp"), "tp"),
        check_vma=False,
    )
```
